32 devices in a mesh: grp: 2 (over x), ep: 8 (over z, y), tp: 2 (over core).
Axes of the slice: x: 2, y: 2, z: 4, core: 2. Of those that a mesh axis runs over, the one named last changes fastest.
Arguments:
- tokens: bfloat16 [512, 2048], P(('grp', 'ep')), parts along dimension 0, may hold values from -6 to 6
- norm_gain: float32 [2048], replicated, may hold values from 0.1 to 1.9
- group_prob: float32 [512], P(('grp', 'ep')), parts along dimension 0, may hold values from 0.5 to 1
- route_logits: float32 [512, 4], P(('grp', 'ep')), parts along dimension 0, may hold values from -6 to 6
- expert_ids: int32 [512, 4], P(('grp', 'ep')), parts along dimension 0, may hold values from 0 to 7, as said below
- w_gate: bfloat16 [8, 2048, 512], P('ep', None, 'tp'), may hold values from -0.125 to 0.125
- w_up: bfloat16 [8, 2048, 512], P('ep', None, 'tp'), may hold values from -0.125 to 0.125
- w_down: bfloat16 [8, 512, 2048], P('ep', 'tp'), may hold values from -0.25 to 0.25
Outputs:
- mixed: bfloat16 [512, 2048], P(('grp', 'ep')), parts along dimension 0
The draws below stay inside these ranges and needn't reach their ends.
There are 2 independent parts, one for each index of `grp`. The reference program is written for one: setup_inputs(seed, part) draws one part's arguments, and reference() takes and returns one part's arrays. A program takes and returns all parts, laid end to end along the dimension named above; an argument that names none is the same for every part. Nothing has to cross between parts.
Inputs may be any that keep to these rules, and one draw needn't show every extreme that they name: `expert_ids`: each token names 4 different experts, all inside one group of 4 consecutive experts. Of the 32 tokens of one index of ep, exactly 16 lie in each group, so at most 16 of them name any one expert; in every draw some expert is named by 16 tokens of every index of ep.
All inputs are finite; a program needn't handle non-finite values.
Results may differ from the reference program's by a relative error of at most 0.0077.
Values may be sent and summed in bfloat16 or wider, within the bound.
A program may use at most 64 MiB of HBM per device.

```python
import jax
import jax.numpy as jnp
from jax import lax

D = 2048
FF = 512
GROUPS = 2
TOP_K = 4
TOK_DEV = 32
EXPERTS = 8
GROUP_SIZE = 4
TOKENS = 256
N_TP = 2


def draw_expert_ids(key, part):
    blocks = TOKENS // TOK_DEV
    keys = jax.random.split(jax.random.fold_in(key, 7), 5)
    labels = jnp.arange(TOK_DEV, dtype=jnp.int32) % GROUPS
    perms = jax.vmap(lambda k: jax.random.permutation(k, labels))(jax.random.split(keys[0], blocks))
    common_hot = jax.random.randint(keys[1], (), 0, GROUP_SIZE)
    hot = jax.random.randint(keys[2], (blocks, GROUPS), 0, GROUP_SIZE)
    hot = hot.at[:, 0].set(common_hot)
    bias = jax.random.randint(keys[3], (GROUPS, GROUP_SIZE), 0, 4) * 32
    noise = jax.random.randint(keys[4], (blocks, TOK_DEV, GROUP_SIZE), 0, 64)
    local = jnp.arange(GROUP_SIZE, dtype=jnp.int32)
    token_bias = bias[perms]
    token_hot = jnp.take_along_axis(hot, perms, axis=1)
    boost = (local[None, None, :] == token_hot[:, :, None]).astype(jnp.int32) * 100000
    scores = (noise + token_bias + boost) * GROUP_SIZE + local[None, None, :]
    unused, picked = lax.top_k(scores, TOP_K)
    ids = perms[:, :, None] * GROUP_SIZE + picked.astype(jnp.int32)
    return ids.reshape(TOKENS, TOP_K).astype(jnp.int32)


def levels(own_key, shape, pieces, low, largest):
    factor_of, own = 1.0, jax.random.fold_in(own_key, 6)
    for position, shards_of in pieces:
        heights = jnp.exp(jax.random.uniform(jax.random.fold_in(own, position), (shards_of,), jnp.float32, low / len(pieces), largest / len(pieces)))
        factor_of = factor_of * jnp.repeat(heights, shape[position] // shards_of).reshape([-1 if axis == position else 1 for axis in range(len(shape))])
    return factor_of


def normal_values(rng, dims, deviation, limit, cuts=(), held_as=jnp.bfloat16):
    factor_of = levels(rng, dims, cuts, -0.22, 0.18) if cuts else 1.0
    drawn = jax.random.normal(rng, dims, jnp.float32) * deviation * factor_of
    return jnp.minimum(jnp.maximum(drawn, -limit), limit).astype(held_as)


def setup_inputs(seed: int = 0, part: int = 0) -> dict:
    arg_keys = jax.random.split(jax.random.key(seed), 9)
    part_keys = jax.random.split(jax.random.fold_in(arg_keys[8], part), 9)
    return {
        "tokens": normal_values(part_keys[0], (TOKENS, D), 1.0, 6.0, ((0, 8),)),
        "norm_gain": jnp.clip(1.0 + 0.18 * jax.random.normal(arg_keys[1], (D,), jnp.float32), 0.1, 1.9),
        "group_prob": jnp.clip(0.5 + 0.5 * jax.random.uniform(part_keys[2], (TOKENS,), jnp.float32) ** levels(part_keys[2], (TOKENS,), ((0, 8),), -0.2, 0.2), 0.5, 1.0),
        "route_logits": normal_values(part_keys[3], (TOKENS, TOP_K), 1.0, 6.0, ((0, 8),), jnp.float32),
        "expert_ids": draw_expert_ids(jax.random.fold_in(jax.random.fold_in(arg_keys[8], part), 71), part),
        "w_gate": normal_values(arg_keys[5], (EXPERTS, D, FF), D ** -0.5, 0.125, ((0, 8), (2, 2))),
        "w_up": normal_values(arg_keys[6], (EXPERTS, D, FF), D ** -0.5, 0.125, ((0, 8), (2, 2))),
        "w_down": normal_values(arg_keys[7], (EXPERTS, FF, D), FF ** -0.5, 0.25, ((0, 8), (1, 2))),
    }


def reference(tokens, norm_gain, group_prob, route_logits, expert_ids, w_gate, w_up, w_down):
    values = tokens.astype(jnp.float32)
    scale = lax.rsqrt(lax.optimization_barrier(jnp.mean(values * values, axis=-1, keepdims=True)) + 1e-06)
    normed = (values * scale * norm_gain).astype(jnp.bfloat16)
    expw = jnp.exp(route_logits)
    route_w = group_prob[:, None] * expw / lax.optimization_barrier(jnp.sum(expw, axis=-1, keepdims=True))
    block = FF // N_TP

    def one_expert(acc, inputs):
        gate_m, up_m, down_m, index = inputs
        gate = jnp.dot(normed, gate_m, preferred_element_type=jnp.float32)
        up = jnp.dot(normed, up_m, preferred_element_type=jnp.float32)
        act = (jax.nn.silu(gate) * up).astype(jnp.bfloat16)
        total = jnp.zeros((normed.shape[0], normed.shape[1]), jnp.float32)
        for piece in range(N_TP):
            part = jnp.dot(act[:, piece * block:(piece + 1) * block], down_m[piece * block:(piece + 1) * block], preferred_element_type=jnp.float32).astype(jnp.bfloat16)
            total = total + lax.optimization_barrier(part).astype(jnp.float32)
        expert_out = lax.optimization_barrier(total.astype(jnp.bfloat16)).astype(jnp.float32)
        weight = lax.optimization_barrier(jnp.sum(route_w * (expert_ids == index).astype(jnp.float32), axis=1))
        return (acc + weight[:, None] * expert_out, None)
    start = jnp.zeros((normed.shape[0], normed.shape[1]), jnp.float32)
    experts = jnp.arange(EXPERTS, dtype=jnp.int32)
    acc, unused = lax.scan(one_expert, start, (w_gate, w_up, w_down, experts))
    return acc.astype(jnp.bfloat16)
```

```python
import functools

import jax
import jax.numpy as jnp
from jax import lax
from jax.experimental import pallas as pl
from jax.experimental.pallas import tpu as pltpu
from jax.sharding import PartitionSpec as P

GROUPS = 2
MESH = pl.DeviceIdType.MESH


def kernel(
    width, n_tp,
    tok_hbm, gain_hbm, prob_hbm, logit_hbm, ids_hbm, wg_hbm, wu_hbm, wd_hbm,
    out_ref,
    tok, gain, prob, logit, ids, wg, wu, wd, send, recv, outs, back, mixed,
    in_sem, wl_sem, ws_sem, wr_sem, ds_sem, dr_sem, bs_sem, br_sem, ms_sem, mr_sem,
):
    e = lax.axis_index("ep")
    q = lax.axis_index("tp")
    sib = n_tp - 1 - q
    gs = width // GROUPS
    nsrc = width // n_tp
    hb = nsrc // GROUPS
    count, dmodel = tok.shape
    cap = count // GROUPS
    topk = ids.shape[0]
    block = e // gs
    mine = (block == q) & (e % n_tp == q)

    smalls = [
        pltpu.make_async_copy(src, dst, in_sem.at[i])
        for i, (src, dst) in enumerate(
            [(tok_hbm, tok), (gain_hbm, gain), (prob_hbm, prob), (logit_hbm, logit), (ids_hbm, ids)]
        )
    ]
    for c in smalls:
        c.start()
    weights = [(wg_hbm, wg), (wu_hbm, wu), (wd_hbm, wd)]
    locals_ = [
        pltpu.make_async_copy(src.at[0], dst.at[q], wl_sem.at[i]) for i, (src, dst) in enumerate(weights)
    ]
    for c in locals_:
        c.start()

    barrier = pltpu.get_barrier_semaphore()
    pl.semaphore_signal(barrier, inc=1, device_id={"tp": sib}, device_id_type=MESH)
    for j in range(gs):
        dest = q * gs + j

        @pl.when(jnp.logical_not(mine & (dest == e)))
        def _():
            pl.semaphore_signal(
                barrier, inc=1, device_id={"ep": dest, "tp": e % n_tp}, device_id_type=MESH
            )

    for i in range(nsrc):
        src = i * n_tp + q

        @pl.when(jnp.logical_not(mine & (src == e)))
        def _():
            pl.semaphore_signal(
                barrier, inc=1, device_id={"ep": src, "tp": block}, device_id_type=MESH
            )

    for c in smalls:
        c.wait()
    values = tok[...].astype(jnp.float32)
    scale = lax.rsqrt(jnp.mean(values * values, axis=-1, keepdims=True) + 1e-06)
    normed = (values * scale * gain[...]).astype(jnp.bfloat16)
    idv = ids[...]
    first = idv[0:1, :]
    grow = jnp.zeros((1, count), jnp.float32)
    for g in range(1, GROUPS):
        grow = grow + jnp.where(first >= g * gs, 1.0, 0.0)
    t_row = lax.broadcasted_iota(jnp.int32, (count, count), 0)
    t_col = lax.broadcasted_iota(jnp.int32, (count, count), 1)
    gfull = jnp.broadcast_to(grow, (count, count))
    gcol = jnp.sum(jnp.where(t_row == t_col, gfull, 0.0), axis=1, keepdims=True)
    same = jnp.where(gfull == gcol, 1.0, 0.0)
    pos_row = jnp.sum(jnp.where(t_row < t_col, same, 0.0), axis=0, keepdims=True)
    pos_col = jnp.sum(jnp.where(t_col < t_row, same, 0.0), axis=1, keepdims=True)
    qf = q.astype(jnp.float32)
    r_io = lax.broadcasted_iota(jnp.int32, (cap, count), 0).astype(jnp.float32)
    place = jnp.where((pos_row == r_io) & (grow == qf), 1.0, 0.0)
    send[...] = jnp.dot(
        place.astype(jnp.bfloat16), normed, preferred_element_type=jnp.float32
    ).astype(jnp.bfloat16)

    @pl.when(mine)
    def _():
        recv[e // n_tp] = send[...]

    wait_n = jnp.where(mine, gs + nsrc - 1, gs + nsrc + 1)
    pl.semaphore_wait(barrier, wait_n)

    def dispatch(j):
        dest = q * gs + j
        return dest, pltpu.make_async_remote_copy(
            src_ref=send,
            dst_ref=recv.at[e // n_tp],
            send_sem=ds_sem.at[j],
            recv_sem=dr_sem.at[e // n_tp],
            device_id={"ep": dest, "tp": e % n_tp},
            device_id_type=MESH,
        )

    for j in range(gs):
        dest, copy = dispatch(j)

        @pl.when(jnp.logical_not(mine & (dest == e)))
        def _():
            copy.start()

    swaps = [
        pltpu.make_async_remote_copy(
            src_ref=src.at[0],
            dst_ref=dst.at[q],
            send_sem=ws_sem.at[i],
            recv_sem=wr_sem.at[i],
            device_id={"tp": sib},
            device_id_type=MESH,
        )
        for i, (src, dst) in enumerate(weights)
    ]
    for c in swaps:
        c.start()

    expw = jnp.exp(logit[...])
    route = prob[...] * expw / jnp.sum(expw, axis=0, keepdims=True)
    expert = lax.broadcasted_iota(jnp.int32, (128, count), 0) + q * gs
    wtok = jnp.zeros((128, count), jnp.float32)
    for k in range(topk):
        wtok = wtok + jnp.where(idv[k : k + 1, :] == expert, route[k : k + 1, :], 0.0)
    wslot = lax.dot_general(
        place, wtok, (((1,), (1,)), ((), ())),
        precision=lax.Precision.HIGHEST, preferred_element_type=jnp.float32,
    )
    s_io = lax.broadcasted_iota(jnp.int32, (count, count), 1).astype(jnp.float32)
    unplace = jnp.where(s_io == gcol * cap + pos_col, 1.0, 0.0).astype(jnp.bfloat16)

    def give(i):
        home = i * n_tp + q
        return home, pltpu.make_async_remote_copy(
            src_ref=outs.at[i],
            dst_ref=back.at[e % gs],
            send_sem=bs_sem.at[i],
            recv_sem=br_sem.at[e % gs],
            device_id={"ep": home, "tp": block},
            device_id_type=MESH,
        )

    for c in locals_:
        c.wait()
    for step in range(GROUPS):
        b = lax.rem(block + step, GROUPS)
        for i in range(hb):
            slot = b * hb + i

            @pl.when(jnp.logical_not(mine & (slot * n_tp + q == e)))
            def _():
                pltpu.make_async_remote_copy(
                    src_ref=send,
                    dst_ref=recv.at[slot],
                    send_sem=ds_sem.at[0],
                    recv_sem=dr_sem.at[slot],
                    device_id={"tp": sib},
                    device_id_type=MESH,
                ).wait_recv()

        def arrived(i):
            if step == 0:
                src, dst = weights[i]
                pltpu.make_async_remote_copy(
                    src_ref=src.at[0],
                    dst_ref=dst.at[sib],
                    send_sem=ws_sem.at[i],
                    recv_sem=wr_sem.at[i],
                    device_id={"tp": sib},
                    device_id_type=MESH,
                ).wait_recv()

        x = recv[pl.ds(b * hb, hb)].reshape(hb * cap, dmodel)
        arrived(0)
        gates = [jnp.dot(x, wg[h], preferred_element_type=jnp.float32) for h in range(n_tp)]
        arrived(1)
        ups = [jnp.dot(x, wu[h], preferred_element_type=jnp.float32) for h in range(n_tp)]
        acts = [((g / (1.0 + jnp.exp(-g))) * u).astype(jnp.bfloat16) for g, u in zip(gates, ups)]
        arrived(2)
        total = jnp.dot(acts[0], wd[0], preferred_element_type=jnp.float32)
        for h in range(1, n_tp):
            total = total + jnp.dot(acts[h], wd[h], preferred_element_type=jnp.float32)
        outs[pl.ds(b * hb, hb)] = total.astype(jnp.bfloat16).reshape(hb, cap, dmodel)
        for i in range(hb):
            slot = b * hb + i
            home, copy = give(slot)

            @pl.when(jnp.logical_not(mine & (home == e)))
            def _():
                copy.start()

            @pl.when(mine & (home == e))
            def _():
                back[e % gs] = outs[slot]

    acc = jnp.zeros((cap, dmodel), jnp.float32)
    for j in range(gs):

        @pl.when(jnp.logical_not(mine & (q * gs + j == e)))
        def _():
            pltpu.make_async_remote_copy(
                src_ref=outs.at[0],
                dst_ref=back.at[j],
                send_sem=bs_sem.at[0],
                recv_sem=br_sem.at[j],
                device_id={"tp": sib},
                device_id_type=MESH,
            ).wait_recv()

        acc = acc + wslot[:, j : j + 1] * back[j].astype(jnp.float32)
    mixed[q] = acc.astype(jnp.bfloat16)
    swap = pltpu.make_async_remote_copy(
        src_ref=mixed.at[q],
        dst_ref=mixed.at[q],
        send_sem=ms_sem,
        recv_sem=mr_sem,
        device_id={"tp": sib},
        device_id_type=MESH,
    )
    swap.start()

    for j in range(gs):
        dest, copy = dispatch(j)

        @pl.when(jnp.logical_not(mine & (dest == e)))
        def _():
            copy.wait_send()

    for c in swaps:
        c.wait_send()
    for i in range(nsrc):
        home, copy = give(i)

        @pl.when(jnp.logical_not(mine & (home == e)))
        def _():
            copy.wait_send()

    pltpu.make_async_remote_copy(
        src_ref=mixed.at[q],
        dst_ref=mixed.at[sib],
        send_sem=ms_sem,
        recv_sem=mr_sem,
        device_id={"tp": sib},
        device_id_type=MESH,
    ).wait_recv()
    swap.wait_send()
    slots = mixed[...].reshape(count, dmodel)
    out_ref[...] = jnp.dot(unplace, slots, preferred_element_type=jnp.float32).astype(jnp.bfloat16)


def shards(tokens, norm_gain, group_prob, route_logits, expert_ids, w_gate, w_up, w_down):
    width = lax.axis_size("ep")
    n_tp = lax.axis_size("tp")
    count, dmodel = tokens.shape
    topk = expert_ids.shape[1]
    ff = w_gate.shape[2]
    cap = count // GROUPS
    gs = width // GROUPS
    nsrc = width // n_tp
    hbm = pl.BlockSpec(memory_space=pltpu.HBM)
    bf, f32 = jnp.bfloat16, jnp.float32
    dma = pltpu.SemaphoreType.DMA
    return pl.pallas_call(
        functools.partial(kernel, width, n_tp),
        out_shape=jax.ShapeDtypeStruct((count, dmodel), bf),
        in_specs=[hbm] * 8,
        out_specs=pl.BlockSpec(memory_space=pltpu.VMEM),
        scratch_shapes=[
            pltpu.VMEM((count, dmodel), bf),
            pltpu.VMEM((1, dmodel), f32),
            pltpu.VMEM((1, count), f32),
            pltpu.VMEM((topk, count), f32),
            pltpu.VMEM((topk, count), jnp.int32),
            pltpu.VMEM((n_tp, dmodel, ff), bf),
            pltpu.VMEM((n_tp, dmodel, ff), bf),
            pltpu.VMEM((n_tp, ff, dmodel), bf),
            pltpu.VMEM((cap, dmodel), bf),
            pltpu.VMEM((nsrc, cap, dmodel), bf),
            pltpu.VMEM((nsrc, cap, dmodel), bf),
            pltpu.VMEM((gs, cap, dmodel), bf),
            pltpu.VMEM((n_tp, cap, dmodel), bf),
            dma((5,)), dma((3,)), dma((3,)), dma((3,)),
            dma((gs,)), dma((nsrc,)), dma((nsrc,)), dma((gs,)),
            dma, dma,
        ],
        compiler_params=pltpu.CompilerParams(collective_id=0, has_side_effects=True),
        name="expert_mixture",
    )(
        tokens, norm_gain.reshape(1, dmodel), group_prob.reshape(1, count), route_logits.T,
        expert_ids.T, w_gate, w_up, w_down,
    )


def solution(mesh):
    in_specs = (
        P(("grp", "ep"), None),
        P(),
        P(("grp", "ep")),
        P(("grp", "ep"), None),
        P(("grp", "ep"), None),
        P("ep", None, "tp"),
        P("ep", None, "tp"),
        P("ep", "tp", None),
    )
    out_specs = P(("grp", "ep"), None)
    return jax.shard_map(shards, mesh=mesh, in_specs=in_specs, out_specs=out_specs, check_vma=False)
```

```python
import functools

import jax
import jax.numpy as jnp
from jax import lax
from jax.experimental import pallas as pl
from jax.experimental.pallas import tpu as pltpu
from jax.sharding import PartitionSpec as P

GROUPS = 2
MESH = pl.DeviceIdType.MESH


def kernel(
    width, n_tp,
    tok_hbm, gain_hbm, prob_hbm, logit_hbm, ids_hbm, wg_hbm, wu_hbm, wd_hbm,
    out_ref,
    tok, gain, prob, logit, ids, wg, wu, wd, send, recv, outs, back, mixed,
    in_sem, wl_sem, ws_sem, wr_sem, ds_sem, dr_sem, bs_sem, br_sem, ms_sem, mr_sem,
):
    e = lax.axis_index("ep")
    q = lax.axis_index("tp")
    sib = n_tp - 1 - q
    gs = width // GROUPS
    nsrc = width // n_tp
    hb = nsrc // GROUPS
    count, dmodel = tok.shape
    cap = count // GROUPS
    topk = ids.shape[0]
    block = e // gs
    mine = (block == q) & (e % n_tp == q)

    smalls = [
        pltpu.make_async_copy(src, dst, in_sem.at[i])
        for i, (src, dst) in enumerate(
            [(tok_hbm, tok), (gain_hbm, gain), (prob_hbm, prob), (logit_hbm, logit), (ids_hbm, ids)]
        )
    ]
    for c in smalls:
        c.start()
    weights = [(wg_hbm, wg), (wu_hbm, wu), (wd_hbm, wd)]
    locals_ = [
        pltpu.make_async_copy(src.at[0], dst.at[q], wl_sem.at[i]) for i, (src, dst) in enumerate(weights)
    ]
    for c in locals_:
        c.start()

    barrier = pltpu.get_barrier_semaphore()
    pl.semaphore_signal(barrier, inc=1, device_id={"tp": sib}, device_id_type=MESH)
    for j in range(gs):
        dest = q * gs + j

        @pl.when(jnp.logical_not(mine & (dest == e)))
        def _():
            pl.semaphore_signal(
                barrier, inc=1, device_id={"ep": dest, "tp": e % n_tp}, device_id_type=MESH
            )

    for i in range(nsrc):
        src = i * n_tp + q

        @pl.when(jnp.logical_not(mine & (src == e)))
        def _():
            pl.semaphore_signal(
                barrier, inc=1, device_id={"ep": src, "tp": block}, device_id_type=MESH
            )

    for c in smalls:
        c.wait()
    values = tok[...].astype(jnp.float32)
    scale = lax.rsqrt(jnp.mean(values * values, axis=-1, keepdims=True) + 1e-06)
    normed = (values * scale * gain[...]).astype(jnp.bfloat16)
    idv = ids[...]
    first = idv[0:1, :]
    grow = jnp.zeros((1, count), jnp.float32)
    for g in range(1, GROUPS):
        grow = grow + jnp.where(first >= g * gs, 1.0, 0.0)
    t_row = lax.broadcasted_iota(jnp.int32, (count, count), 0)
    t_col = lax.broadcasted_iota(jnp.int32, (count, count), 1)
    gfull = jnp.broadcast_to(grow, (count, count))
    gcol = jnp.sum(jnp.where(t_row == t_col, gfull, 0.0), axis=1, keepdims=True)
    same = jnp.where(gfull == gcol, 1.0, 0.0)
    pos_row = jnp.sum(jnp.where(t_row < t_col, same, 0.0), axis=0, keepdims=True)
    pos_col = jnp.sum(jnp.where(t_col < t_row, same, 0.0), axis=1, keepdims=True)
    qf = q.astype(jnp.float32)
    r_io = lax.broadcasted_iota(jnp.int32, (cap, count), 0).astype(jnp.float32)
    place = jnp.where((pos_row == r_io) & (grow == qf), 1.0, 0.0)
    send[...] = jnp.dot(
        place.astype(jnp.bfloat16), normed, preferred_element_type=jnp.float32
    ).astype(jnp.bfloat16)

    @pl.when(mine)
    def _():
        recv[e // n_tp] = send[...]

    wait_n = jnp.where(mine, gs + nsrc - 1, gs + nsrc + 1)
    pl.semaphore_wait(barrier, wait_n)

    def dispatch(j):
        dest = q * gs + j
        return dest, pltpu.make_async_remote_copy(
            src_ref=send,
            dst_ref=recv.at[e // n_tp],
            send_sem=ds_sem.at[j],
            recv_sem=dr_sem.at[e // n_tp],
            device_id={"ep": dest, "tp": e % n_tp},
            device_id_type=MESH,
        )

    for j in range(gs):
        dest, copy = dispatch(j)

        @pl.when(jnp.logical_not(mine & (dest == e)))
        def _():
            copy.start()

    swaps = [
        pltpu.make_async_remote_copy(
            src_ref=src.at[0],
            dst_ref=dst.at[q],
            send_sem=ws_sem.at[i],
            recv_sem=wr_sem.at[i],
            device_id={"tp": sib},
            device_id_type=MESH,
        )
        for i, (src, dst) in enumerate(weights)
    ]
    for c in swaps:
        c.start()

    expw = jnp.exp(logit[...])
    route = prob[...] * expw / jnp.sum(expw, axis=0, keepdims=True)
    expert = lax.broadcasted_iota(jnp.int32, (128, count), 0) + q * gs
    wtok = jnp.zeros((128, count), jnp.float32)
    for k in range(topk):
        wtok = wtok + jnp.where(idv[k : k + 1, :] == expert, route[k : k + 1, :], 0.0)
    wslot = lax.dot_general(
        place, wtok, (((1,), (1,)), ((), ())),
        precision=lax.Precision.HIGHEST, preferred_element_type=jnp.float32,
    )
    s_io = lax.broadcasted_iota(jnp.int32, (count, count), 1).astype(jnp.float32)
    unplace = jnp.where(s_io == gcol * cap + pos_col, 1.0, 0.0).astype(jnp.bfloat16)

    def give(i):
        home = i * n_tp + q
        return home, pltpu.make_async_remote_copy(
            src_ref=outs.at[i],
            dst_ref=back.at[e % gs],
            send_sem=bs_sem.at[i],
            recv_sem=br_sem.at[e % gs],
            device_id={"ep": home, "tp": block},
            device_id_type=MESH,
        )

    for c in locals_:
        c.wait()
    for step in range(GROUPS):
        b = lax.rem(block + step, GROUPS)
        for i in range(hb):
            slot = b * hb + i

            @pl.when(jnp.logical_not(mine & (slot * n_tp + q == e)))
            def _():
                pltpu.make_async_remote_copy(
                    src_ref=send,
                    dst_ref=recv.at[slot],
                    send_sem=ds_sem.at[0],
                    recv_sem=dr_sem.at[slot],
                    device_id={"tp": sib},
                    device_id_type=MESH,
                ).wait_recv()

        def arrived(i):
            if step == 0:
                src, dst = weights[i]
                pltpu.make_async_remote_copy(
                    src_ref=src.at[0],
                    dst_ref=dst.at[sib],
                    send_sem=ws_sem.at[i],
                    recv_sem=wr_sem.at[i],
                    device_id={"tp": sib},
                    device_id_type=MESH,
                ).wait_recv()

        x = recv[pl.ds(b * hb, hb)].reshape(hb * cap, dmodel)
        arrived(0)
        gates = [jnp.dot(x, wg[h], preferred_element_type=jnp.float32) for h in range(n_tp)]
        arrived(1)
        ups = [jnp.dot(x, wu[h], preferred_element_type=jnp.float32) for h in range(n_tp)]
        acts = [((g / (1.0 + jnp.exp(-g))) * u).astype(jnp.bfloat16) for g, u in zip(gates, ups)]
        arrived(2)
        total = jnp.dot(acts[0], wd[0], preferred_element_type=jnp.float32)
        for h in range(1, n_tp):
            total = total + jnp.dot(acts[h], wd[h], preferred_element_type=jnp.float32)
        outs[pl.ds(b * hb, hb)] = total.astype(jnp.bfloat16).reshape(hb, cap, dmodel)
        for i in range(hb):
            slot = b * hb + i
            home, copy = give(slot)

            @pl.when(jnp.logical_not(mine & (home == e)))
            def _():
                copy.start()

            @pl.when(mine & (home == e))
            def _():
                back[e % gs] = outs[slot]

    acc = jnp.zeros((cap, dmodel), jnp.float32)
    for j in range(gs):

        @pl.when(jnp.logical_not(mine & (q * gs + j == e)))
        def _():
            pltpu.make_async_remote_copy(
                src_ref=outs.at[0],
                dst_ref=back.at[j],
                send_sem=bs_sem.at[0],
                recv_sem=br_sem.at[j],
                device_id={"tp": sib},
                device_id_type=MESH,
            ).wait_recv()

        acc = acc + wslot[:, j : j + 1] * back[j].astype(jnp.float32)
    mixed[q] = acc.astype(jnp.bfloat16)
    swap = pltpu.make_async_remote_copy(
        src_ref=mixed.at[q],
        dst_ref=mixed.at[q],
        send_sem=ms_sem,
        recv_sem=mr_sem,
        device_id={"tp": sib},
        device_id_type=MESH,
    )
    swap.start()

    for j in range(gs):
        dest, copy = dispatch(j)

        @pl.when(jnp.logical_not(mine & (dest == e)))
        def _():
            copy.wait_send()

    for c in swaps:
        c.wait_send()
    for i in range(nsrc):
        home, copy = give(i)

        @pl.when(jnp.logical_not(mine & (home == e)))
        def _():
            copy.wait_send()

    pltpu.make_async_remote_copy(
        src_ref=mixed.at[q],
        dst_ref=mixed.at[sib],
        send_sem=ms_sem,
        recv_sem=mr_sem,
        device_id={"tp": sib},
        device_id_type=MESH,
    ).wait_recv()
    swap.wait_send()
    slots = mixed[...].reshape(count, dmodel)
    out_ref[...] = jnp.dot(unplace, slots, preferred_element_type=jnp.float32).astype(jnp.bfloat16)


def shards(tokens, norm_gain, group_prob, route_logits, expert_ids, w_gate, w_up, w_down):
    width = lax.axis_size("ep")
    n_tp = lax.axis_size("tp")
    count, dmodel = tokens.shape
    topk = expert_ids.shape[1]
    ff = w_gate.shape[2]
    cap = count // GROUPS
    gs = width // GROUPS
    nsrc = width // n_tp
    hbm = pl.BlockSpec(memory_space=pltpu.HBM)
    bf, f32 = jnp.bfloat16, jnp.float32
    dma = pltpu.SemaphoreType.DMA
    return pl.pallas_call(
        functools.partial(kernel, width, n_tp),
        out_shape=pltpu.VMEM((count, dmodel), bf),
        in_specs=[hbm] * 8,
        out_specs=pl.BlockSpec(memory_space=pltpu.VMEM),
        scratch_shapes=[
            pltpu.VMEM((count, dmodel), bf),
            pltpu.VMEM((1, dmodel), f32),
            pltpu.VMEM((1, count), f32),
            pltpu.VMEM((topk, count), f32),
            pltpu.VMEM((topk, count), jnp.int32),
            pltpu.VMEM((n_tp, dmodel, ff), bf),
            pltpu.VMEM((n_tp, dmodel, ff), bf),
            pltpu.VMEM((n_tp, ff, dmodel), bf),
            pltpu.VMEM((cap, dmodel), bf),
            pltpu.VMEM((nsrc, cap, dmodel), bf),
            pltpu.VMEM((nsrc, cap, dmodel), bf),
            pltpu.VMEM((gs, cap, dmodel), bf),
            pltpu.VMEM((n_tp, cap, dmodel), bf),
            dma((5,)), dma((3,)), dma((3,)), dma((3,)),
            dma((gs,)), dma((nsrc,)), dma((nsrc,)), dma((gs,)),
            dma, dma,
        ],
        compiler_params=pltpu.CompilerParams(collective_id=0, has_side_effects=True),
        name="expert_mixture",
    )(
        tokens, norm_gain.reshape(1, dmodel), group_prob.reshape(1, count), route_logits.T,
        expert_ids.T, w_gate, w_up, w_down,
    )


def solution(mesh):
    in_specs = (
        P(("grp", "ep"), None),
        P(),
        P(("grp", "ep")),
        P(("grp", "ep"), None),
        P(("grp", "ep"), None),
        P("ep", None, "tp"),
        P("ep", None, "tp"),
        P("ep", "tp", None),
    )
    out_specs = P(("grp", "ep"), None)
    return jax.shard_map(shards, mesh=mesh, in_specs=in_specs, out_specs=out_specs, check_vma=False)
```
